32 devices in a mesh: sp: 8 (over z, core), tp: 4 (over y, x).
Axes of the slice: x: 2, y: 2, z: 4, core: 2. Of those that a mesh axis runs over, the one named last changes fastest.
Arguments:
- residual: bfloat16 [2048, 2048], P('sp'), may hold values from -6 to 6
- queries: bfloat16 [2048, 16, 128], P('sp', 'tp'), may hold values from -256 to 256
- key_vectors: bfloat16 [2048, 16, 128], P('sp', 'tp'), may hold values from -5.3 to 5.3
- value_rows: bfloat16 [2048, 16, 128], P('sp', 'tp'), may hold values from -6 to 6
- head_lambda: float32 [16], P('tp'), may hold values from 0.3 to 0.8
- head_gain: float32 [128], replicated, may hold values from 0.1 to 1.9
- out_weight: bfloat16 [2048, 2048], P('tp'), may hold values from -0.125 to 0.125
- ffn_gain: float32 [2048], replicated, may hold values from 0.1 to 1.9
- expert_gate: bfloat16 [8, 2048, 4096], P('sp', None, 'tp'), may hold values from -0.125 to 0.125
- expert_up: bfloat16 [8, 2048, 4096], P('sp', None, 'tp'), may hold values from -0.125 to 0.125
- expert_down: bfloat16 [8, 4096, 2048], P('sp', None, 'tp'), may hold values from -0.09375 to 0.09375
- routing: int32 [2048, 2], P('sp'), may hold values from 0 to 7, as said below
- route_weight: float32 [2048, 2], P('sp'), may hold values from 0.1 to 0.9
Outputs:
- layer_out: bfloat16 [2048, 2048], P('sp')
The draws below stay inside these ranges and needn't reach their ends.
Inputs may be any that keep to these rules, and one draw needn't show every extreme that they name: `routing`: each row names two different experts of one group of 2 consecutive experts. In each aligned block of 256 rows no expert is named by more than 128 rows, and in every block some expert is named by exactly 128 rows.
All inputs are finite; a program needn't handle non-finite values.
Results may differ from the reference program's by a relative error of at most 0.015.
Values may be sent and summed in bfloat16 or wider, within the bound.
A program may use at most 64 MiB of HBM per device.

```python
import math
import jax
import jax.numpy as jnp
from jax import lax

D = 2048
HEADS = 16
QK = 64
HV = 128
FF = 4096
GROUPS = 4
TOP = 2
T_SP = 256
SEQ = 2048
EXPERTS = 8
CAP = 128
N_SP = 8


def drawn(key):
    spread = 1.3
    base_key, query_key = jax.random.split(jax.random.fold_in(key, 5), 2)
    width = 2 * QK
    key_array = spread * jax.random.truncated_normal(base_key, -4.0, 4.0, (SEQ, HEADS, width), jnp.float32)
    query_array = spread * jax.random.truncated_normal(query_key, -4.0, 4.0, (SEQ, HEADS, width), jnp.float32)
    return (query_array, key_array)


def draw_queries(key, part):
    return drawn(key)[0].astype(jnp.bfloat16)


def draw_key_vectors(key, part):
    return drawn(key)[1].astype(jnp.bfloat16)


def draw_routing(key, part):
    per_group = EXPERTS // GROUPS
    block_count = SEQ // T_SP
    order_key, inner_key, rank_key = jax.random.split(jax.random.fold_in(key, 11), 3)
    group_order = jax.random.permutation(order_key, GROUPS).astype(jnp.int32)
    inner_order = jax.vmap(lambda sub_key: jax.random.permutation(sub_key, per_group))(jax.random.split(inner_key, GROUPS)).astype(jnp.int32)
    rank_table = jax.vmap(lambda sub_key: jax.random.permutation(sub_key, T_SP))(jax.random.split(rank_key, block_count)).astype(jnp.int32).reshape(-1)
    half_mark = T_SP // 2
    rank_level = (rank_table >= half_mark).astype(jnp.int32) + (rank_table >= half_mark + T_SP // 4).astype(jnp.int32) + (rank_table >= half_mark + T_SP // 4 + T_SP // 8).astype(jnp.int32)
    offsets = jnp.array([0, T_SP // 2, 3 * T_SP // 4, 7 * T_SP // 8], jnp.int32)
    within = rank_table - offsets[rank_level]
    first_pick = within % per_group
    step_size = 1 + within // per_group % max(per_group - 1, 1)
    second_pick = (first_pick + step_size) % per_group
    group_id = group_order[rank_level]
    first_expert = group_id * per_group + inner_order[group_id, first_pick]
    second_expert = group_id * per_group + inner_order[group_id, second_pick]
    return jnp.stack([first_expert, second_expert], axis=1).astype(jnp.int32)


def block_levels(rng, shape, shards, least, high):
    loudness = 1.0
    for axis_at, parts in shards:
        draws = jax.random.uniform(jax.random.fold_in(jax.random.fold_in(rng, 6), axis_at), (parts,), jnp.float32, least / len(shards), high / len(shards))
        loudness = loudness * jnp.repeat(jnp.exp(draws), shape[axis_at] // parts).reshape((-1,) + (1,) * (len(shape) - 1 - axis_at))
    return loudness


def scatter_about(rng, extent, scale, most, cuts=(), held_as=jnp.bfloat16):
    level = block_levels(rng, extent, cuts, -0.22, 0.18) if cuts else 1.0
    drawn = jax.random.normal(rng, extent, jnp.float32) * scale * level
    return jnp.minimum(jnp.maximum(drawn, -most), most).astype(held_as)


def setup_inputs(seed: int = 0) -> dict:
    keys = jax.random.split(jax.random.key(seed), 14)
    residual = scatter_about(keys[0], (SEQ, D), 1.0, 6.0, ((0, 8),))
    queries = draw_queries(jax.random.fold_in(keys[13], 71), 0)
    key_vectors = draw_key_vectors(jax.random.fold_in(keys[13], 71), 0)
    value_rows = scatter_about(keys[3], (SEQ, HEADS, HV), 1.0, 6.0, ((0, 8), (1, 4)))
    head_lambda = jnp.clip(0.3 + 0.5 * jax.random.uniform(keys[4], (HEADS,), jnp.float32) ** block_levels(keys[4], (HEADS,), ((0, 4),), -0.2, 0.2), 0.3, 0.8)
    head_gain = jnp.clip(1.0 + 0.18 * jax.random.normal(keys[5], (HV,), jnp.float32), 0.1, 1.9)
    out_weight = scatter_about(keys[6], (HEADS * HV, D), (HEADS * HV) ** -0.5, 0.125, ((0, 4),))
    ffn_gain = jnp.clip(1.0 + 0.18 * jax.random.normal(keys[7], (D,), jnp.float32), 0.1, 1.9)
    expert_gate = scatter_about(keys[8], (EXPERTS, D, FF), D ** -0.5, 0.125, ((0, 8), (2, 4)))
    expert_up = scatter_about(keys[9], (EXPERTS, D, FF), D ** -0.5, 0.125, ((0, 8), (2, 4)))
    expert_down = scatter_about(keys[10], (EXPERTS, FF, D), FF ** -0.5, 0.09375, ((0, 8), (2, 4)))
    routing = draw_routing(jax.random.fold_in(keys[13], 71), 0)
    route_weight = jnp.clip(0.1 + 0.79999997 * jax.random.uniform(keys[12], (SEQ, TOP), jnp.float32) ** block_levels(keys[12], (SEQ, TOP), ((0, 8),), -0.2, 0.2), 0.1, 0.9)
    return {"residual": residual, "queries": queries, "key_vectors": key_vectors, "value_rows": value_rows, "head_lambda": head_lambda, "head_gain": head_gain, "out_weight": out_weight, "ffn_gain": ffn_gain, "expert_gate": expert_gate, "expert_up": expert_up, "expert_down": expert_down, "routing": routing, "route_weight": route_weight}


norm_eps = 1e-06

def differential(queries, key_vectors, value_rows, head_lambda, head_gain):
    seq_len = queries.shape[0]
    block_len = math.gcd(seq_len, 512)
    score_scale = QK ** (-0.5)
    key_float = key_vectors.astype(jnp.float32)
    value_float = value_rows.astype(jnp.float32)
    key_pos = jnp.arange(seq_len, dtype=jnp.int32)

    def one_map(query_part, key_part, query_pos):
        scores = jnp.einsum('qhd,khd->hqk', query_part, key_part) * score_scale
        masked = jnp.where(key_pos[None, None, :] <= query_pos[None, :, None], scores, -jnp.inf)
        highest = lax.optimization_barrier(jnp.max(masked, axis=-1, keepdims=True))
        weights = jnp.exp(masked - highest)
        totals = lax.optimization_barrier(jnp.sum(weights, axis=-1))
        rounded = lax.optimization_barrier(weights.astype(jnp.bfloat16)).astype(jnp.float32)
        blended = jnp.einsum('hqk,khe->qhe', rounded, value_float)
        return blended / jnp.transpose(totals)[:, :, None]

    def one_block(block_index):
        first_row = block_index * block_len
        query_rows = lax.dynamic_slice_in_dim(queries, first_row, block_len, 0).astype(jnp.float32)
        query_pos = first_row + jnp.arange(block_len, dtype=jnp.int32)
        first_map = one_map(query_rows[:, :, :QK], key_float[:, :, :QK], query_pos)
        second_map = one_map(query_rows[:, :, QK:], key_float[:, :, QK:], query_pos)
        return first_map - head_lambda[None, :, None] * second_map
    blocks_out = lax.map(one_block, jnp.arange(seq_len // block_len, dtype=jnp.int32))
    combined = blocks_out.reshape(seq_len, HEADS, HV)
    normed = combined * lax.rsqrt(lax.optimization_barrier(jnp.mean(combined * combined, axis=-1, keepdims=True)) + norm_eps) * head_gain
    return normed.astype(jnp.bfloat16).reshape(seq_len, HEADS * HV)

def reference(residual, queries, key_vectors, value_rows, head_lambda, head_gain, out_weight, ffn_gain, expert_gate, expert_up, expert_down, routing, route_weight):
    attended = differential(queries, key_vectors, value_rows, head_lambda, head_gain)
    stream = residual.astype(jnp.float32) + jnp.dot(attended, out_weight, preferred_element_type=jnp.float32)
    normed = (stream * lax.rsqrt(lax.optimization_barrier(jnp.mean(stream * stream, axis=-1, keepdims=True)) + norm_eps) * ffn_gain).astype(jnp.bfloat16)
    slot_count = N_SP * CAP

    def expert_step(totals, stacked):
        gate_weight, up_weight, down_weight, expert_id = stacked
        chosen = jnp.any(routing == expert_id, axis=1)
        token_ids = jnp.nonzero(chosen, size=slot_count, fill_value=0)[0].astype(jnp.int32)
        live_slot = jnp.arange(slot_count, dtype=jnp.int32) < jnp.sum(chosen.astype(jnp.int32))
        picked = normed[token_ids]
        gate_part = jnp.dot(picked, gate_weight, preferred_element_type=jnp.float32)
        up_part = jnp.dot(picked, up_weight, preferred_element_type=jnp.float32)
        inner_act = (jax.nn.silu(gate_part) * up_part).astype(jnp.bfloat16)
        result = jnp.dot(inner_act, down_weight, preferred_element_type=jnp.float32).astype(jnp.bfloat16)
        factor = lax.optimization_barrier(jnp.sum(jnp.where(routing[token_ids] == expert_id, route_weight[token_ids], jnp.zeros_like(route_weight[token_ids])), axis=1))
        factor = jnp.where(live_slot, factor, jnp.zeros_like(factor))
        return (totals.at[token_ids].add(factor[:, None] * result.astype(jnp.float32)), None)
    moe_sum, _ = lax.scan(expert_step, jnp.zeros((SEQ, D), jnp.float32), (expert_gate, expert_up, expert_down, jnp.arange(EXPERTS, dtype=jnp.int32)))
    return (stream + moe_sum).astype(jnp.bfloat16)
```

```python
import functools
import math

import jax
import jax.numpy as jnp
from jax import lax
from jax.experimental import pallas as pl
from jax.experimental.pallas import tpu as pltpu
from jax.sharding import PartitionSpec as P

GROUPS = 4


norm_eps = 1e-06


def online_update(running, query_part, key_part, value_part, query_pos, key_pos, score_scale):
    highest, totals, accum = running
    scores = (
        jnp.einsum("qhd,khd->hqk", query_part, key_part, preferred_element_type=jnp.float32)
        * score_scale
    )
    scores = jnp.where(key_pos[None, None, :] <= query_pos[None, :, None], scores, -jnp.inf)
    new_high = jnp.maximum(highest, jnp.max(scores, axis=-1))
    shrink = jnp.exp(highest - new_high)
    weights = jnp.exp(scores - new_high[:, :, None])
    totals = shrink * totals + jnp.sum(weights, axis=-1)
    blended = jnp.einsum(
        "hqk,khe->qhe", weights.astype(jnp.bfloat16), value_part, preferred_element_type=jnp.float32
    )
    accum = jnp.transpose(shrink)[:, :, None] * accum + blended
    return (new_high, totals, accum)


def shards(
    residual,
    queries,
    key_vectors,
    value_rows,
    head_lambda,
    head_gain,
    out_weight,
    ffn_gain,
    expert_gate,
    expert_up,
    expert_down,
    routing,
    route_weight,
):
    tok_count = queries.shape[0]
    local_heads = queries.shape[1]
    half_width = queries.shape[2] // 2
    value_width = value_rows.shape[2]
    score_scale = half_width ** (-0.5)
    query_pos = lax.axis_index("sp") * tok_count + jnp.arange(tok_count, dtype=jnp.int32)
    last_query = query_pos[-1]
    first_half = queries[:, :, :half_width]
    second_half = queries[:, :, half_width:]
    start_high = jnp.full((local_heads, tok_count), -1e30, jnp.float32)
    start_total = jnp.zeros((local_heads, tok_count), jnp.float32)
    start_accum = jnp.zeros((tok_count, local_heads, value_width), jnp.float32)
    empty_state = (start_high, start_total, start_accum)
    running = (empty_state, empty_state)
    key_piece = lax.all_gather(key_vectors, "sp", axis=0, tiled=True)
    value_piece = lax.all_gather(value_rows, "sp", axis=0, tiled=True)
    piece_len = key_piece.shape[0]
    block_len = math.gcd(piece_len, 512)
    block_count = piece_len // block_len
    key_blocks = key_piece.reshape(block_count, block_len, local_heads, 2 * half_width)
    value_blocks = value_piece.reshape(block_count, block_len, local_heads, value_width)

    def visit(current, stacked):
        block_index, key_block, value_block = stacked
        block_first = block_index * block_len
        key_pos = block_first + jnp.arange(block_len, dtype=jnp.int32)

        def compute(inside):
            first_state = online_update(
                inside[0],
                first_half,
                key_block[:, :, :half_width],
                value_block,
                query_pos,
                key_pos,
                score_scale,
            )
            second_state = online_update(
                inside[1],
                second_half,
                key_block[:, :, half_width:],
                value_block,
                query_pos,
                key_pos,
                score_scale,
            )
            return (first_state, second_state)

        return (lax.cond(block_first <= last_query, compute, lambda inside: inside, current), None)

    running, _ = lax.scan(
        visit, running, (jnp.arange(block_count, dtype=jnp.int32), key_blocks, value_blocks)
    )
    first_state, second_state = running
    first_out = first_state[2] / jnp.transpose(first_state[1])[:, :, None]
    second_out = second_state[2] / jnp.transpose(second_state[1])[:, :, None]
    combined = first_out - head_lambda[None, :, None] * second_out
    normed_heads = (
        combined
        * lax.rsqrt(jnp.mean(combined * combined, axis=-1, keepdims=True) + norm_eps)
        * head_gain
    )
    attended = normed_heads.astype(jnp.bfloat16).reshape(tok_count, local_heads * value_width)
    partial_proj = jnp.dot(attended, out_weight, preferred_element_type=jnp.float32)
    projected = lax.psum(partial_proj.astype(jnp.bfloat16), "tp").astype(jnp.float32)
    stream = residual.astype(jnp.float32) + projected
    block_normed = (
        stream * lax.rsqrt(jnp.mean(stream * stream, axis=-1, keepdims=True) + norm_eps) * ffn_gain
    ).astype(jnp.bfloat16)
    expert_count = lax.axis_size("sp")
    tp_count = lax.axis_size("tp")
    per_group = expert_count // GROUPS
    capacity = tok_count // per_group
    top_count = routing.shape[1]
    model_width = block_normed.shape[1]
    flat_routes = routing.reshape(-1)
    route_count = flat_routes.shape[0]
    onehot = (flat_routes[:, None] == jnp.arange(expert_count, dtype=jnp.int32)[None, :]).astype(
        jnp.int32
    )
    earlier = jnp.cumsum(onehot, axis=0) - onehot
    position = jnp.sum(earlier * onehot, axis=1)
    slot_index = flat_routes * capacity + position
    slot_token = (
        jnp.full((expert_count * capacity,), tok_count, jnp.int32)
        .at[slot_index]
        .set(jnp.arange(route_count, dtype=jnp.int32) // top_count)
    )
    slot_table = slot_token.reshape(expert_count, capacity)
    slice_width = model_width // tp_count
    own_columns = lax.dynamic_slice_in_dim(
        block_normed, lax.axis_index("tp") * slice_width, slice_width, 1
    )
    outgoing = jnp.take(own_columns, slot_table, axis=0, mode="fill", fill_value=0)
    landed = lax.all_to_all(outgoing, "sp", split_axis=0, concat_axis=0, tiled=True)
    arrived = lax.all_gather(landed, "tp", axis=2, tiled=True)
    expert_rows = arrived.reshape(-1, model_width)
    gate_part = jnp.dot(expert_rows, expert_gate[0], preferred_element_type=jnp.float32)
    up_part = jnp.dot(expert_rows, expert_up[0], preferred_element_type=jnp.float32)
    inner_act = (jax.nn.silu(gate_part) * up_part).astype(jnp.bfloat16)
    down_width = expert_down.shape[2]
    weight_rows = expert_down[0]
    expert_sum = jnp.dot(
        lax.all_gather(inner_act, "tp", axis=1, tiled=True),
        weight_rows,
        preferred_element_type=jnp.float32,
    )
    expert_out = expert_sum.astype(jnp.bfloat16).reshape(expert_count, capacity, down_width)
    returned = lax.all_to_all(expert_out, "sp", split_axis=0, concat_axis=0, tiled=True)
    per_route = returned.reshape(expert_count * capacity, down_width)[slot_index]
    weighted = per_route.astype(jnp.float32) * route_weight.reshape(-1)[:, None]
    token_sum = jnp.sum(weighted.reshape(tok_count, top_count, down_width), axis=1)
    moe_rows = lax.all_gather(token_sum.astype(jnp.bfloat16), "tp", axis=1, tiled=True).astype(
        token_sum.dtype
    )
    return (stream + moe_rows).astype(jnp.bfloat16)


MESH = pl.DeviceIdType.MESH
F32 = jnp.float32
BF16 = jnp.bfloat16


def remote(src, dst, send_sem, recv_sem, sp, tp):
    return pltpu.make_async_remote_copy(
        src_ref=src,
        dst_ref=dst,
        send_sem=send_sem,
        recv_sem=recv_sem,
        device_id={"sp": sp, "tp": tp},
        device_id_type=MESH,
    )


def mixed_dot(left, right, contract):
    return lax.dot_general(left, right, (contract, ((), ())), preferred_element_type=F32)


def attention_kernel(
    n, tps, heads, head_width,
    q_ref, kv_ref, wt_ref, wd_ref, lam_ref, gain_ref, ow_ref, res_ref, fg_ref,
    stream_ref, normed_ref, wdr_ref, wtall_ref,
    kvall, qs, highs, totals, acc, att, part, rbuf, sq_send, sq_recv,
    local_sem, kv_next, kv_sib, kv_recv, wd_send, wd_recv, wt_send, wt_recv,
    rs_send, rs_recv, sq_ss, sq_rs,
):
    sp = lax.axis_index("sp")
    tp = lax.axis_index("tp")
    z, c = sp // 2, sp % 2
    zs = n // 2
    sib = 2 * z + 1 - c
    toks = q_ref.shape[0]
    width = heads * head_width
    half = head_width // 2
    own = pltpu.make_async_copy(kv_ref, kvall.at[sp], local_sem)
    own.start()
    wd_rows = wd_ref.shape[0] // tps

    def wd_copy(d):
        to = (tp + d) % tps
        return remote(
            wd_ref.at[pl.ds(pl.multiple_of(to * wd_rows, wd_rows), wd_rows), :],
            wdr_ref.at[tp], wd_send.at[d], wd_recv.at[d], sp, to,
        )

    def wt_copy(d):
        return remote(wt_ref, wtall_ref.at[sp], wt_send.at[d], wt_recv.at[d], (sp + d) % n, tp)

    for d in range(1, n):
        wt_copy(d).start()
    for d in range(1, tps):
        wd_copy(d).start()
    wtall_ref[sp] = wt_ref[...]

    lane = lax.broadcasted_iota(jnp.int32, (toks, head_width), 1)
    scale = half ** (-0.5)
    for h in range(heads):
        block = q_ref[:, h * head_width : (h + 1) * head_width].astype(F32) * scale
        qs[2 * h] = jnp.where(lane < half, block, 0.0).astype(BF16)
        qs[2 * h + 1] = jnp.where(lane >= half, block, 0.0).astype(BF16)
    highs[...] = jnp.full_like(highs, -1e30)
    totals[...] = jnp.zeros_like(totals)
    acc[...] = jnp.zeros_like(acc)
    rows = lax.broadcasted_iota(jnp.int32, (toks, toks), 0)
    cols = lax.broadcasted_iota(jnp.int32, (toks, toks), 1)

    def process(b):
        seen = cols + b * toks <= rows + sp * toks
        for h in range(heads):
            keys = kvall[b, :, h * head_width : (h + 1) * head_width]
            vals = kvall[b, :, width + h * head_width : width + (h + 1) * head_width]
            for u in (2 * h, 2 * h + 1):
                scores = mixed_dot(qs[u], keys, ((1,), (1,)))
                scores = jnp.where(seen, scores, -1e30)
                old = highs[u]
                high = jnp.maximum(old, jnp.max(scores, axis=1, keepdims=True))
                shrink = jnp.exp(old - high)
                weights = jnp.exp(scores - high)
                totals[u] = shrink * totals[u] + jnp.sum(weights, axis=1, keepdims=True)
                blended = mixed_dot(weights.astype(BF16), vals, ((1,), (0,)))
                acc[u] = shrink * acc[u] + blended
                highs[u] = high

    def next_copy(b):
        return remote(kvall.at[b], kvall.at[b], kv_next.at[b], kv_recv.at[b], sp + 2, tp)

    def sib_copy(b):
        return remote(kvall.at[b], kvall.at[b], kv_sib.at[b], kv_recv.at[b], sib, tp)

    own.wait()

    def visit(j, carry):
        b = 2 * (z - j) + c
        other = 2 * (z - j) + 1 - c

        @pl.when(j > 0)
        def _():
            sib_copy(b).wait_recv()

        @pl.when(z < zs - 1)
        def _():
            next_copy(b).start()

        @pl.when(jnp.logical_or(j > 0, c == 0))
        def _():
            sib_copy(b).start()

        process(b)

        @pl.when(jnp.logical_or(j > 0, c == 1))
        def _():
            sib_copy(other).wait_recv()
            process(other)

        return carry

    lax.fori_loop(0, z + 1, visit, 0)

    for h in range(heads):
        first = acc[2 * h] / totals[2 * h]
        second = acc[2 * h + 1] / totals[2 * h + 1]
        mix = first - lam_ref[h] * second
        mix = mix * lax.rsqrt(jnp.mean(mix * mix, axis=1, keepdims=True) + norm_eps) * gain_ref[...]
        att[:, h * head_width : (h + 1) * head_width] = mix.astype(BF16)
    piece = ow_ref.shape[1] // tps

    def projected(to):
        return jnp.dot(
            att[...], ow_ref[:, pl.ds(pl.multiple_of(to * piece, piece), piece)],
            preferred_element_type=F32,
        )

    def rs_copy(d):
        return remote(
            part.at[d], rbuf.at[d], rs_send.at[d], rs_recv.at[d], sp, (tp + d) % tps
        )

    for d in range(1, tps):
        part[d] = projected((tp + d) % tps).astype(BF16)
        rs_copy(d).start()
    mine = pl.ds(pl.multiple_of(tp * piece, piece), piece)
    total = projected(tp)
    for d in range(1, tps):
        rs_copy(d).wait_recv()
        total = total + rbuf[d].astype(F32)
    stream = res_ref[:, mine].astype(F32) + total
    stream_ref[...] = stream
    eye = rows == cols
    squares = jnp.sum(stream * stream, axis=1, keepdims=True)
    as_row = jnp.sum(jnp.where(eye, squares, 0.0), axis=0, keepdims=True)
    sq_send[...] = jnp.broadcast_to(as_row, sq_send.shape)

    def sq_copy(d):
        return remote(
            sq_send, sq_recv.at[d], sq_ss.at[d], sq_rs.at[d], sp, (tp + d) % tps
        )

    for d in range(1, tps):
        sq_copy(d).start()
    for d in range(1, tps):
        sq_copy(d).wait_recv()
        as_row = as_row + sq_recv[d, 0:1, :]
    as_col = jnp.sum(jnp.where(eye, as_row, 0.0), axis=1, keepdims=True)
    mean = as_col * (1.0 / (piece * tps))
    normed_ref[...] = (stream * lax.rsqrt(mean + norm_eps) * fg_ref[:, mine]).astype(BF16)

    for d in range(1, tps):
        sq_copy(d).wait_send()
        rs_copy(d).wait_send()
        wd_copy(d).wait()
    for d in range(1, n):
        wt_copy(d).wait()

    def drain(j, carry):
        b = 2 * (z - j) + c

        @pl.when(z < zs - 1)
        def _():
            next_copy(b).wait_send()

        @pl.when(jnp.logical_or(j > 0, c == 0))
        def _():
            sib_copy(b).wait_send()

        return carry

    lax.fori_loop(0, z + 1, drain, 0)


def expert_kernel(
    n, tps, cap,
    normed_ref, stream_ref, sel_ref, selt_ref, wtall_ref, gate_ref, up_ref, wd_ref, wdr_ref,
    out_ref,
    xs, xall, wg, wu, wdv, hid, keep, away, near, rsend, rrecv, back, ret,
    w_sem, x_send, x_tp, x_sib, x_recv, n_send, n_recv, r_send, r_recv, b_send, b_recv,
    o_send, o_recv,
):
    sp = lax.axis_index("sp")
    tp = lax.axis_index("tp")
    z, c = sp // 2, sp % 2
    zs = n // 2
    sib = 2 * z + 1 - c
    piece = normed_ref.shape[1]
    wd_rows = wdv.shape[1]
    loads = [
        pltpu.make_async_copy(gate_ref.at[0], wg, w_sem.at[0]),
        pltpu.make_async_copy(up_ref.at[0], wu, w_sem.at[1]),
        pltpu.make_async_copy(
            wd_ref.at[pl.ds(pl.multiple_of(tp * wd_rows, wd_rows), wd_rows), :],
            wdv.at[tp], w_sem.at[2],
        ),
    ]
    for d in range(1, tps):
        peer = (tp + d) % tps
        loads.append(pltpu.make_async_copy(wdr_ref.at[peer], wdv.at[peer], w_sem.at[2 + d]))
    for load in loads:
        load.start()

    def spot(src, core, part):
        return xall.at[
            src,
            pl.ds(pl.multiple_of(core * cap, cap), cap),
            pl.ds(pl.multiple_of(part * piece, piece), piece),
        ]

    def x_copy(s):
        group = (z + s) % zs
        return remote(
            xs.at[s], spot(z, c, tp), x_send.at[s], x_recv.at[z, c, tp], 2 * group + c, tp
        )

    def x_wait(src, core, part):
        here = spot(src, core, part)
        remote(here, here, x_send.at[0], x_recv.at[src, core, part], sib, tp).wait_recv()

    def tp_copy(src, d):
        here = spot(src, c, tp)
        return remote(
            here, here, x_tp.at[src, d], x_recv.at[src, c, tp], sp, (tp + d) % tps
        )

    def sib_copy(src, part):
        here = spot(src, c, part)
        return remote(here, here, x_sib.at[src, part], x_recv.at[src, c, part], sib, tp)

    for s in list(range(1, zs)) + [0]:
        group = (z + s) % zs
        picked = jnp.dot(
            sel_ref[pl.ds(pl.multiple_of(group * cap, cap), cap), :], normed_ref[...],
            preferred_element_type=F32,
        ).astype(BF16)
        if s:
            xs[s] = picked
            x_copy(s).start()
        else:
            spot(z, c, tp)[...] = picked

    def origin(s):
        return (z - s + zs) % zs

    def arrive(s):
        src = origin(s)

        @pl.when(s > 0)
        def _():
            x_wait(src, c, tp)

        for d in range(1, tps):
            tp_copy(src, d).start()
        sib_copy(src, tp).start()

    def complete(s):
        src = origin(s)
        for d in range(1, tps):
            x_wait(src, c, (tp + d) % tps)
            sib_copy(src, (tp + d) % tps).start()
        for part in range(tps):
            x_wait(src, 1 - c, part)

    def near_copy(src):
        return remote(away.at[src], near.at[src], n_send.at[src], n_recv.at[src], sib, tp)

    tile = 256
    eye = lax.broadcasted_iota(jnp.int32, (cap, cap), 0) == lax.broadcasted_iota(
        jnp.int32, (cap, cap), 1
    )
    experts = wtall_ref.shape[1]
    which = lax.broadcasted_iota(jnp.int32, (experts, cap), 0)

    def weight_col(src, core):
        table = wtall_ref[2 * src + core]
        row = jnp.sum(jnp.where(which == sp, table, 0.0), axis=0, keepdims=True)
        return jnp.sum(jnp.where(eye, row, 0.0), axis=1, keepdims=True)

    def ffn(s):
        src = origin(s)

        def one(i, carry):
            at = pl.ds(pl.multiple_of(i * tile, tile), tile)
            x = xall[src]
            gate = jnp.dot(x, wg[:, at], preferred_element_type=F32)
            up = jnp.dot(x, wu[:, at], preferred_element_type=F32)
            hid[:, at] = (gate / (1.0 + jnp.exp(-gate)) * up).astype(BF16)
            return carry

        lax.fori_loop(0, wg.shape[1] // tile, one, 0)
        keep_w = weight_col(src, c)
        away_w = weight_col(src, 1 - c)
        keep_rows = pl.ds(pl.multiple_of(c * cap, cap), cap)
        away_rows = pl.ds(pl.multiple_of((1 - c) * cap, cap), cap)

        def two(j, carry):
            away[src, j] = (
                jnp.dot(hid[away_rows, :], wdv[j], preferred_element_type=F32) * away_w
            ).astype(BF16)
            keep[src, j] = jnp.dot(hid[keep_rows, :], wdv[j], preferred_element_type=F32) * keep_w
            return carry

        lax.fori_loop(0, tps, two, 0)
        near_copy(src).start()

    def r_copy(src, d):
        return remote(
            rsend.at[src, d], rrecv.at[src, d], r_send.at[src, d], r_recv.at[src, d],
            sp, (tp + d) % tps,
        )

    def spread(s):
        src = origin(s)
        near_copy(src).wait_recv()
        for d in range(1, tps):
            to = (tp + d) % tps
            rsend[src, d] = (keep[src, to] + near[src, to].astype(F32)).astype(BF16)
            r_copy(src, d).start()

    def b_copy(src):
        return remote(
            back.at[src], ret.at[z], b_send.at[src], b_recv.at[z], 2 * src + c, tp
        )

    def finish(s):
        src = origin(s)
        total = keep[src, tp] + near[src, tp].astype(F32)
        for d in range(1, tps):
            r_copy(src, d).wait_recv()
            total = total + rrecv[src, d].astype(F32)

        @pl.when(s == 0)
        def _():
            ret[z] = total.astype(BF16)

        @pl.when(s > 0)
        def _():
            back[src] = total.astype(BF16)
            b_copy(src).start()

    arrive(0)
    for load in loads:
        load.wait()

    def step(s, carry):
        pl.when(s + 1 < zs)(lambda: arrive(s + 1))

        @pl.when(s < zs)
        def _():
            complete(s)
            ffn(s)

        pl.when(jnp.logical_and(s >= 1, s <= zs))(lambda: spread(s - 1))
        pl.when(s >= 2)(lambda: finish(s - 2))
        return carry

    lax.fori_loop(0, zs + 2, step, 0)

    for s in range(1, zs):
        group = (z + s) % zs
        remote(
            back.at[group], ret.at[group], b_send.at[group], b_recv.at[group], sib, tp
        ).wait_recv()
    rows = ret[...].reshape(zs * cap, piece)
    layer = stream_ref[...] + jnp.dot(selt_ref[...], rows, preferred_element_type=F32)
    mine = out_ref.at[:, pl.ds(pl.multiple_of(tp * piece, piece), piece)]
    mine[...] = layer.astype(BF16)

    def o_copy(d):
        return remote(mine, mine, o_send.at[d], o_recv.at[d], sp, (tp + d) % tps)

    for d in range(1, tps):
        o_copy(d).start()
    for s in range(1, zs):
        x_copy(s).wait_send()
        b_copy(origin(s)).wait_send()
    for src in range(zs):
        near_copy(src).wait_send()
        sib_copy(src, tp).wait_send()
        for d in range(1, tps):
            tp_copy(src, d).wait_send()
            sib_copy(src, (tp + d) % tps).wait_send()
            r_copy(src, d).wait_send()
    for d in range(1, tps):
        o_copy(d).wait()


def paired_shards(
    residual, queries, key_vectors, value_rows, head_lambda, head_gain, out_weight, ffn_gain,
    expert_gate, expert_up, expert_down, routing, route_weight,
):
    n = lax.axis_size("sp")
    tps = lax.axis_size("tp")
    toks, heads, head_width = queries.shape
    width = heads * head_width
    model = residual.shape[1]
    piece = model // tps
    experts = n
    per_group = experts // GROUPS
    cap = toks // per_group
    group = routing[:, 0] // per_group
    member = (group[:, None] == jnp.arange(GROUPS, dtype=jnp.int32)[None, :]).astype(jnp.int32)
    position = jnp.sum((jnp.cumsum(member, axis=0) - member) * member, axis=1)
    slot = group * cap + position
    slots = jnp.arange(GROUPS * cap, dtype=jnp.int32)
    sel = (slots[:, None] == slot[None, :]).astype(BF16)
    selt = (slot[:, None] == slots[None, :]).astype(BF16)
    by_expert = jnp.sum(
        jnp.where(
            routing[:, :, None] == jnp.arange(experts, dtype=jnp.int32), route_weight[:, :, None], 0.0
        ),
        axis=1,
    )
    table = jnp.einsum(
        "gst,tgp->gps",
        sel.astype(F32).reshape(GROUPS, cap, toks),
        by_expert.reshape(toks, GROUPS, per_group),
        precision=lax.Precision.HIGHEST,
    ).reshape(experts, cap)
    kv = jnp.concatenate(
        [key_vectors.reshape(toks, width), value_rows.reshape(toks, width)], axis=1
    )
    down = expert_down[0]
    wd_rows = down.shape[0] // tps
    vmem = pl.BlockSpec(memory_space=pltpu.VMEM)
    smem = pl.BlockSpec(memory_space=pltpu.SMEM)
    hbm = pl.BlockSpec(memory_space=pl.ANY)
    dma = pltpu.SemaphoreType.DMA
    units = 2 * heads
    stream, normed, wdr, wtall = pl.pallas_call(
        functools.partial(attention_kernel, n, tps, heads, head_width),
        out_shape=(
            jax.ShapeDtypeStruct((toks, piece), F32),
            jax.ShapeDtypeStruct((toks, piece), BF16),
            jax.ShapeDtypeStruct((tps, wd_rows, piece), BF16),
            jax.ShapeDtypeStruct((n, experts, cap), F32),
        ),
        in_specs=[vmem, hbm, vmem, hbm, smem, vmem, vmem, vmem, vmem],
        out_specs=(vmem, vmem, hbm, vmem),
        scratch_shapes=[
            pltpu.VMEM((n, toks, 2 * width), BF16),
            pltpu.VMEM((units, toks, head_width), BF16),
            pltpu.VMEM((units, toks, 1), F32),
            pltpu.VMEM((units, toks, 1), F32),
            pltpu.VMEM((units, toks, head_width), F32),
            pltpu.VMEM((toks, width), BF16),
            pltpu.VMEM((tps, toks, piece), BF16),
            pltpu.VMEM((tps, toks, piece), BF16),
            pltpu.VMEM((8, toks), F32),
            pltpu.VMEM((tps, 8, toks), F32),
            dma,
            dma((n,)), dma((n,)), dma((n,)),
            dma((tps,)), dma((tps,)), dma((n,)), dma((n,)),
            dma((tps,)), dma((tps,)), dma((tps,)), dma((tps,)),
        ],
        compiler_params=pltpu.CompilerParams(has_side_effects=True),
        name="attend",
    )(
        queries.reshape(toks, width), kv, table, down, head_lambda, head_gain.reshape(1, -1),
        out_weight, residual, ffn_gain.reshape(1, -1),
    )
    zs = n // 2
    return pl.pallas_call(
        functools.partial(expert_kernel, n, tps, cap),
        out_shape=jax.ShapeDtypeStruct((toks, model), BF16),
        in_specs=[vmem, vmem, vmem, vmem, vmem, hbm, hbm, hbm, hbm],
        out_specs=vmem,
        scratch_shapes=[
            pltpu.VMEM((zs, cap, piece), BF16),
            pltpu.VMEM((zs, 2 * cap, model), BF16),
            pltpu.VMEM(expert_gate.shape[1:], BF16),
            pltpu.VMEM(expert_up.shape[1:], BF16),
            pltpu.VMEM((tps, wd_rows, piece), BF16),
            pltpu.VMEM((2 * cap, expert_gate.shape[2]), BF16),
            pltpu.VMEM((zs, tps, cap, piece), F32),
            pltpu.VMEM((zs, tps, cap, piece), BF16),
            pltpu.VMEM((zs, tps, cap, piece), BF16),
            pltpu.VMEM((zs, tps, cap, piece), BF16),
            pltpu.VMEM((zs, tps, cap, piece), BF16),
            pltpu.VMEM((zs, cap, piece), BF16),
            pltpu.VMEM((zs, cap, piece), BF16),
            dma((2 + tps,)),
            dma((zs,)), dma((zs, tps)), dma((zs, tps)), dma((zs, 2, tps)),
            dma((zs,)), dma((zs,)), dma((zs, tps)), dma((zs, tps)),
            dma((zs,)), dma((zs,)), dma((tps,)), dma((tps,)),
        ],
        compiler_params=pltpu.CompilerParams(has_side_effects=True),
        name="experts",
    )(normed, stream, sel, selt, wtall, expert_gate, expert_up, down, wdr)


def solution(mesh):
    in_specs = (
        P("sp", None),
        P("sp", "tp", None),
        P("sp", "tp", None),
        P("sp", "tp", None),
        P("tp"),
        P(),
        P("tp", None),
        P(),
        P("sp", None, "tp"),
        P("sp", None, "tp"),
        P("sp", None, "tp"),
        P("sp", None),
        P("sp", None),
    )
    out_specs = P("sp", None)
    paired = mesh.shape["sp"] == 2 * GROUPS
    return jax.shard_map(paired_shards if paired else shards, mesh=mesh, in_specs=in_specs, out_specs=out_specs, check_vma=False)
```
